32 devices in a mesh: sp: 8 (over z, x), tp: 4 (over y, core).
Axes of the slice: x: 2, y: 2, z: 4, core: 2. Of those that a mesh axis runs over, the one named last changes fastest.
Arguments:
- in_gate: bfloat16 [1024, 2048], P('tp', 'sp'), may hold values from -6 to 6
- out_gate: bfloat16 [1024, 2048], P('tp', 'sp'), may hold values from -6 to 6
- values: bfloat16 [1024, 2048], P('tp', 'sp'), may hold values from -6 to 6
- conv_taps: bfloat16 [3, 1024], P(None, 'tp'), may hold values from -3.5 to 3.5
- doc_ids: int32 [2048], P('sp'), may hold values from 0 to 1, as said below
- residual: bfloat16 [2048, 2048], P('sp'), may hold values from -6 to 6
- out_weight: bfloat16 [1024, 2048], P('tp'), may hold values from -0.1875 to 0.1875
- norm_gain: bfloat16 [2048], replicated, may hold values from 0.099609375 to 1.8984375
- routes: int32 [2048, 2], P('sp'), may hold values from 0 to 7, all different within a row; in each aligned block of 256 rows (0 to 255, 256 to 511, ...) at most 96 rows name the same one
- route_weights: float32 [2048, 2], P('sp'), may hold values from 0.2 to 1
- expert_gate: bfloat16 [8, 2048, 4224], P('sp', None, 'tp'), may hold values from -0.125 to 0.125
- expert_up: bfloat16 [8, 2048, 4224], P('sp', None, 'tp'), may hold values from -0.125 to 0.125
- expert_down: bfloat16 [8, 4224, 2048], P('sp', 'tp'), may hold values from -0.09375 to 0.09375
Outputs:
- merged: bfloat16 [2048, 2048], P('sp', 'tp')
The draws below stay inside these ranges and needn't reach their ends.
Inputs may be any that keep to these rules, and one draw needn't show every extreme that they name: `routes`: each row names 2 different experts. Within the rows of one index of sp (aligned blocks of 256 rows) no expert is named more than 96 times, a bound that some expert reaches in some blocks. `doc_ids`: never falls along the sequence; starts at 0 and rises by one at each of 1 document starts, each number used.
All inputs are finite; a program needn't handle non-finite values.
Results may differ from the reference program's by a relative error of at most 0.019.
Values may be sent and summed in bfloat16 or wider, within the bound.
No kernel may reach another device: no remote copies, remote signals or barrier semaphores. Data moves between devices by JAX's collectives and lax.ppermute only.
A program may use at most 64 MiB of HBM per device.

```python
import math
import jax
import jax.numpy as jnp
import numpy as np
from jax import lax

D = 2048
D_CONV = 1024
FF = 4224
TOP = 2
TOK_SP = 256
TOKENS = 2048
EXPERTS = 8
CAP = 96
DOCS = 2
N_SP = 8
N_TP = 4


def draw_doc_ids(key, part):
    starts = jax.random.permutation(jax.random.fold_in(key, 17), TOKENS - 1)[:DOCS - 1].astype(jnp.int32) + 1
    positions = jnp.arange(TOKENS, dtype=jnp.int32)
    return jnp.sum((positions[:, None] >= starts[None, :]).astype(jnp.int32), axis=1).astype(jnp.int32)


def shard_levels(key, extent, cuts, low, largest):
    factor_of = 1.0
    for axis_at, blocks in cuts:
        heights = jax.random.uniform(jax.random.fold_in(jax.random.fold_in(key, 6), axis_at), (blocks,), jnp.float32, low / len(cuts), largest / len(cuts))
        factor_of = factor_of * jnp.repeat(jnp.exp(heights), extent[axis_at] // blocks).reshape((-1,) + (1,) * (len(extent) - 1 - axis_at))
    return factor_of


def assign_block(own_key, own, number, rows, number_of, top, reach, slope):
    order = jax.random.permutation(own_key, number_of)
    crowded, usual = shares(number_of, rows * top, reach, slope, True), shares(number_of, rows * top, reach, slope, False)
    places = jnp.arange(number_of)

    def named(sizes, offset_by):
        used = int((sizes > 0).sum())
        fixed = max(1, used // 4)
        moved = fixed + (places - fixed + offset_by * (used - fixed)) % max(1, number_of - fixed)
        return jnp.zeros((number_of,), jnp.int32).at[order[jnp.where(places < fixed, places, moved)]].set(jnp.asarray(sizes, jnp.int32))

    sizes = jnp.where(number % 4 == 0, named(crowded, number // 4), named(usual, number - number // 4 - 1))
    mixed = jax.random.permutation(jax.random.fold_in(own, 3), number_of)
    source_of, sink = mixed[0:number_of // 2 * 2:2], mixed[1:number_of // 2 * 2:2]
    room = jnp.minimum(sizes[source_of] - 1, reach - sizes[sink]) // 2
    room = jnp.where((source_of == order[0]) | (sink == order[0]) | (sizes[sink] == 0), 0, jnp.maximum(room, 0))
    moved = jax.random.randint(jax.random.fold_in(own, 4), (number_of // 2,), 0, 1 << 20) % (room + 1)
    sizes = sizes.at[source_of].add(-moved).at[sink].add(moved)
    labels = jnp.searchsorted(jnp.cumsum(sizes), jnp.arange(rows * top), side="right").astype(jnp.int32)
    grid = labels.reshape(top, rows).T
    grid = grid[jax.random.permutation(jax.random.fold_in(own, 1), rows)]
    offset_by = jax.random.randint(jax.random.fold_in(own, 2), (rows, 1), 0, top)
    return jnp.take_along_axis(grid, (jnp.arange(top)[None, :] + offset_by) % top, axis=1)


def shares(number_of, total, reach, slope, full):
    portions = [(1 << 20) // math.isqrt(grade ** slope) + 1 for grade in range(1, number_of + 1)]
    largest = reach if full else min(reach, max(-(-total // number_of), total * portions[0] // sum(portions)))
    least = 1 if total - largest >= number_of - 1 else 0
    given, rest = [largest] + [least] * (number_of - 1), total - largest - least * (number_of - 1)
    while rest > 0:
        candidates = [i for i in range(1, number_of) if given[i] < largest] or [i for i in range(1, number_of) if given[i] < reach]
        mass, budget = sum([portions[i] for i in candidates]), rest
        for i in candidates:
            more = min(reach - given[i], max(1, budget * portions[i] // mass), rest)
            given[i] = given[i] + more
            rest = rest - more
    return np.array(given)


def centred(key, extent, deviation, most, shards=(), kind=jnp.bfloat16):
    result = deviation * jax.random.normal(key, extent, jnp.float32)
    if shards:
        result = result * shard_levels(key, extent, shards, -0.22, 0.18)
    return jnp.clip(result, -most, most).astype(kind)


def setup_inputs(seed: int = 0) -> dict:
    key_list = jax.random.split(jax.random.key(seed), 14)
    in_gate = centred(key_list[0], (D_CONV, TOKENS), 1.0, 6.0, ((0, 4), (1, 8)))
    out_gate = centred(key_list[1], (D_CONV, TOKENS), 1.0, 6.0, ((0, 4), (1, 8)))
    values = centred(key_list[2], (D_CONV, TOKENS), 1.0, 6.0, ((0, 4), (1, 8)))
    conv_taps = centred(key_list[3], (3, D_CONV), 3 ** -0.5, 3.5, ((1, 4),))
    doc_ids = draw_doc_ids(jax.random.fold_in(key_list[13], 71), 0)
    residual = centred(key_list[5], (TOKENS, D), 1.0, 6.0, ((0, 8),))
    out_weight = centred(key_list[6], (D_CONV, D), D_CONV ** -0.5, 0.1875, ((0, 4),))
    norm_gain = jnp.clip(1.0 + 0.18 * jax.random.normal(key_list[7], (D,), jnp.float32), 0.099609375, 1.8984375).astype(jnp.bfloat16)
    routes_keys = jax.random.split(jax.random.fold_in(key_list[8], 1), TOKENS // TOK_SP)
    routes_turns = jax.random.permutation(jax.random.fold_in(key_list[8], 3), TOKENS // TOK_SP)
    routes = jax.vmap(lambda own, number: assign_block(jax.random.fold_in(key_list[8], 2), own, number, TOK_SP, EXPERTS, TOP, CAP, 1))(routes_keys, routes_turns).reshape((TOKENS, TOP))
    route_weights = jnp.clip(0.2 + 0.8 * jax.random.uniform(key_list[9], (TOKENS, TOP), jnp.float32) ** shard_levels(key_list[9], (TOKENS, TOP), ((0, 8),), -0.2, 0.2), 0.2, 1.0)
    expert_gate = centred(key_list[10], (EXPERTS, D, FF), D ** -0.5, 0.125, ((0, 8), (2, 4)))
    expert_up = centred(key_list[11], (EXPERTS, D, FF), D ** -0.5, 0.125, ((0, 8), (2, 4)))
    expert_down = centred(key_list[12], (EXPERTS, FF, D), FF ** -0.5, 0.09375, ((0, 8), (1, 4)))
    return {"in_gate": in_gate, "out_gate": out_gate, "values": values, "conv_taps": conv_taps, "doc_ids": doc_ids, "residual": residual, "out_weight": out_weight, "norm_gain": norm_gain, "routes": routes, "route_weights": route_weights, "expert_gate": expert_gate, "expert_up": expert_up, "expert_down": expert_down}


EPSILON = 1e-06

def reference(in_gate, out_gate, values, conv_taps, doc_ids, residual, out_weight, norm_gain, routes, route_weights, expert_gate, expert_up, expert_down):
    gated_in = (in_gate.astype(jnp.float32) * values.astype(jnp.float32)).astype(jnp.bfloat16)
    gated_f = lax.optimization_barrier(gated_in).astype(jnp.float32)
    length = doc_ids.shape[0]
    shift_one = jnp.pad(gated_f, ((0, 0), (1, 0)))[:, :length]
    shift_two = jnp.pad(gated_f, ((0, 0), (2, 0)))[:, :length]
    docs_one = jnp.pad(doc_ids, (1, 0), constant_values=-1)[:length]
    docs_two = jnp.pad(doc_ids, (2, 0), constant_values=-1)[:length]
    near_mask = (docs_one == doc_ids).astype(jnp.float32)
    far_mask = (docs_two == doc_ids).astype(jnp.float32)
    tap_values = conv_taps.astype(jnp.float32)
    convolved = tap_values[2][:, None] * gated_f + tap_values[1][:, None] * shift_one * near_mask[None, :] + tap_values[0][:, None] * shift_two * far_mask[None, :]
    mixed_rows = (out_gate.astype(jnp.float32) * convolved).astype(jnp.bfloat16)
    projected = jnp.dot(mixed_rows.T, out_weight, preferred_element_type=jnp.float32)
    stream = residual.astype(jnp.float32) + projected
    inv_rms = lax.rsqrt(lax.optimization_barrier(jnp.mean(stream * stream, axis=1, keepdims=True)) + EPSILON)
    normed = (stream * inv_rms * norm_gain.astype(jnp.float32)[None, :]).astype(jnp.bfloat16)
    total_rows = N_SP * CAP
    hidden_block = FF // N_TP

    def one_expert(expert):
        hit_table = routes == expert
        weight_row = lax.optimization_barrier(jnp.sum(jnp.where(hit_table, route_weights, jnp.float32(0.0)), axis=1))
        used_rows = jnp.any(hit_table, axis=1)
        picked = jnp.nonzero(used_rows, size=total_rows, fill_value=0)[0].astype(jnp.int32)
        live_rows = (jnp.arange(total_rows) < jnp.sum(used_rows.astype(jnp.int32))).astype(jnp.float32)
        row_block = jnp.take(normed, picked, axis=0)
        gate_sum = jnp.dot(row_block, expert_gate[expert], preferred_element_type=jnp.float32)
        up_sum = jnp.dot(row_block, expert_up[expert], preferred_element_type=jnp.float32)
        hidden = (jax.nn.silu(gate_sum) * up_sum).astype(jnp.bfloat16)
        pieces = jnp.einsum('rnf,nfd->nrd', hidden.astype(jnp.float32).reshape(total_rows, N_TP, hidden_block), expert_down[expert].astype(jnp.float32).reshape(N_TP, hidden_block, D))
        pieces = lax.optimization_barrier(pieces.astype(jnp.bfloat16)).astype(jnp.float32)
        summed = lax.optimization_barrier(lax.optimization_barrier(jnp.sum(pieces, axis=0)).astype(jnp.bfloat16)).astype(jnp.float32)
        return (picked, (jnp.take(weight_row, picked) * live_rows)[:, None] * summed)
    picked_all, terms = lax.map(one_expert, jnp.arange(EXPERTS, dtype=jnp.int32))
    blended = jnp.zeros_like(stream).at[picked_all.reshape(-1)].add(terms.reshape(-1, D))
    return (stream + blended).astype(jnp.bfloat16)
```

```python
import jax
import jax.numpy as jnp
from jax import lax
from jax.experimental import pallas as pl
from jax.experimental.pallas import tpu as pltpu
from jax.sharding import PartitionSpec as P

EPSILON = 1e-06
CHUNKS = 2


def shifted(x, axis, by):
    count = lax.axis_size(axis)
    pairs = [(i, i + by) for i in range(count) if 0 <= i + by < count]
    return lax.ppermute(x, axis, pairs)


def rotated(x, axis, by):
    count = lax.axis_size(axis)
    return lax.ppermute(x, axis, [(i, (i + by) % count) for i in range(count)])


def other_core(x):
    return lax.ppermute(x, "tp", [(i, i ^ 1) for i in range(lax.axis_size("tp"))])


def next_chip(x, by):
    count = lax.axis_size("tp")
    return lax.ppermute(x, "tp", [(i, (i + 2 * by) % count) for i in range(count)])


def expert_kernel(order_ref, *refs):
    pieces = len(refs) - 9
    x_refs = refs[:pieces]
    gain_ref, gate_ref, up_ref, down_ref, out_ref = refs[pieces : pieces + 5]
    rows_ref, gate_acc, up_acc, hidden_ref = refs[pieces + 5 :]
    step = pl.program_id(0)
    width = x_refs[0].shape[1]

    @pl.when(step == 0)
    def _():
        total = sum(
            jnp.sum(jnp.square(x[...].astype(jnp.float32)), axis=1, keepdims=True) for x in x_refs
        )
        inv_rms = lax.rsqrt(total / (pieces * width) + EPSILON)
        for j, x in enumerate(x_refs):
            rows_ref[j] = (
                x[...].astype(jnp.float32) * inv_rms * gain_ref[order_ref[j]].astype(jnp.float32)
            ).astype(jnp.bfloat16)

    @pl.when(step < pieces)
    def _():
        rows = rows_ref[step]
        contract = (((1,), (1,)), ((), ()))
        gate_part = lax.dot_general(
            rows, gate_ref[...], contract, preferred_element_type=jnp.float32
        )
        up_part = lax.dot_general(rows, up_ref[...], contract, preferred_element_type=jnp.float32)

        @pl.when(step == 0)
        def _():
            gate_acc[...] = gate_part
            up_acc[...] = up_part

        @pl.when(step > 0)
        def _():
            gate_acc[...] += gate_part
            up_acc[...] += up_part

    @pl.when(step == pieces - 1)
    def _():
        gate_sum = gate_acc[...]
        hidden_ref[...] = (gate_sum / (1.0 + jnp.exp(-gate_sum)) * up_acc[...]).astype(jnp.bfloat16)

    @pl.when(step >= pieces)
    def _():
        out_ref[0] = jnp.dot(
            hidden_ref[...], down_ref[...], preferred_element_type=jnp.float32
        ).astype(jnp.bfloat16)


def expert_rows(order, xs, gain, gate_t, up_t, down):
    pieces = len(xs)
    rows, width = xs[0].shape
    units = gate_t.shape[0]
    whole = pl.BlockSpec((rows, width), lambda i, o: (0, 0))
    first = pl.BlockSpec((units, width), lambda i, o: (0, o[jnp.minimum(i, pieces - 1)]))
    last = pl.BlockSpec(
        (units, width), lambda i, o: (0, o[pieces + jnp.maximum(i - pieces, 0)])
    )
    return pl.pallas_call(
        expert_kernel,
        out_shape=jax.ShapeDtypeStruct((pieces, rows, width), jnp.bfloat16),
        grid_spec=pltpu.PrefetchScalarGridSpec(
            num_scalar_prefetch=1,
            grid=(2 * pieces,),
            in_specs=[whole] * pieces
            + [pl.BlockSpec((pieces, 1, width), lambda i, o: (0, 0, 0)), first, first, last],
            out_specs=pl.BlockSpec(
                (1, rows, width), lambda i, o: (jnp.maximum(i - pieces, 0), 0, 0)
            ),
            scratch_shapes=[
                pltpu.VMEM((pieces, rows, width), jnp.bfloat16),
                pltpu.VMEM((rows, units), jnp.float32),
                pltpu.VMEM((rows, units), jnp.float32),
                pltpu.VMEM((rows, units), jnp.bfloat16),
            ],
        ),
        cost_estimate=pl.CostEstimate(
            flops=6 * rows * units * pieces * width,
            bytes_accessed=6 * units * pieces * width,
            transcendentals=rows * units,
        ),
        compiler_params=pltpu.CompilerParams(dimension_semantics=("arbitrary",)),
    )(order, *xs, gain, gate_t, up_t, down)


def shards(
    in_gate,
    out_gate,
    values,
    conv_taps,
    doc_ids,
    residual,
    out_weight,
    norm_gain,
    routes,
    route_weights,
    expert_gate,
    expert_up,
    expert_down,
):
    bf16, f32 = jnp.bfloat16, jnp.float32
    tp_count = lax.axis_size("tp")
    chips = tp_count // 2
    experts = lax.axis_size("sp")
    me = lax.axis_index("tp")
    chip, core = me // 2, me % 2
    tokens, top_count = routes.shape
    length = doc_ids.shape[0]
    model_width = residual.shape[1]
    width = model_width // tp_count

    gated_in = (in_gate.astype(f32) * values.astype(f32)).astype(bf16)
    edge = jnp.concatenate(
        [gated_in[:, -2:], jnp.broadcast_to(doc_ids[-2:].astype(bf16)[None, :], (16, 2))], axis=0
    )
    edge = shifted(edge, "sp", 1)
    channels = gated_in.shape[0]
    tail_rows, tail_docs = edge[:channels], edge[channels].astype(jnp.int32)
    extended = lax.optimization_barrier(jnp.concatenate([tail_rows, gated_in], axis=1)).astype(f32)
    docs_ext = jnp.concatenate([tail_docs, doc_ids])
    near_mask = (docs_ext[1 : length + 1] == doc_ids).astype(f32)
    far_mask = (docs_ext[0:length] == doc_ids).astype(f32)
    taps = conv_taps.astype(f32)
    convolved = (
        taps[2][:, None] * extended[:, 2:]
        + taps[1][:, None] * extended[:, 1 : length + 1] * near_mask[None, :]
        + taps[0][:, None] * extended[:, 0:length] * far_mask[None, :]
    )
    mixed_rows = (out_gate.astype(f32) * convolved).astype(bf16)
    partial = lax.dot_general(
        mixed_rows, out_weight, (((0,), (0,)), ((), ())), preferred_element_type=f32
    ).astype(bf16)

    def of_core(which):
        even = jnp.concatenate(
            [partial[:, (2 * y) * width : (2 * y + 1) * width] for y in range(chips)], axis=1
        )
        odd = jnp.concatenate(
            [partial[:, (2 * y + 1) * width : (2 * y + 2) * width] for y in range(chips)], axis=1
        )
        return jnp.where(which == 0, even, odd)

    from_core = other_core(of_core(1 - core))
    chip_sum = of_core(core).astype(f32) + from_core.astype(f32)

    def of_chip(which):
        return lax.dynamic_slice_in_dim(chip_sum, which * width, width, 1)

    projected = of_chip(chip)
    for by in range(1, chips):
        projected = projected + next_chip(of_chip((chip + by) % chips).astype(bf16), by).astype(f32)
    stream = (
        lax.dynamic_slice_in_dim(residual, me * width, width, 1).astype(f32) + projected
    )

    capacity = 3 * tokens * top_count // (2 * experts)
    part = capacity // CHUNKS
    names = jnp.arange(experts, dtype=jnp.int32)
    hits = sum((routes[:, k : k + 1] == names[None, :]).astype(f32) for k in range(top_count))
    positions = jnp.arange(tokens, dtype=jnp.int32)
    before = (positions[None, :] < positions[:, None]).astype(bf16)
    earlier = jnp.dot(before, hits.astype(bf16), preferred_element_type=f32)
    away = (routes - lax.axis_index("sp")) % experts
    slots = []
    for k in range(top_count):
        rank = jnp.sum(
            jnp.where(routes[:, k : k + 1] == names[None, :], earlier, 0.0), axis=1
        ).astype(jnp.int32)
        slots.append((rank // part) * (experts * part) + away[:, k] * part + rank % part)
    slot_count = experts * capacity
    places = jnp.arange(slot_count, dtype=jnp.int32)
    pick = sum((slot[None, :] == places[:, None]).astype(f32) for slot in slots).astype(bf16)
    put = jnp.concatenate(
        [(slot[:, None] == places[None, :]) for slot in slots], axis=0
    ).astype(bf16)
    pick, put = lax.optimization_barrier((pick, put))

    stream_low = stream.astype(bf16)
    steps = jnp.arange(chips, dtype=jnp.int32)
    came_from = ((chip - steps) % chips) * 2
    goes_to = ((chip + steps) % chips) * 2
    order = jnp.concatenate(
        [came_from + core, came_from + (1 - core), goes_to + (1 - core), goes_to + core]
    ).astype(jnp.int32)
    gain = norm_gain.reshape(tp_count, 1, width)
    gate_t = expert_gate[0].T
    up_t = expert_up[0].T
    down = expert_down[0]

    size = experts * part
    returned = []
    for chunk in range(CHUNKS):
        picked = jnp.dot(
            pick[chunk * size : (chunk + 1) * size], stream_low, preferred_element_type=f32
        ).astype(bf16)
        blocks = [picked[:part]] + [
            rotated(picked[d * part : (d + 1) * part], "sp", d) for d in range(1, experts)
        ]
        own = jnp.concatenate(blocks, axis=0)
        near = [own] + [next_chip(own, by) for by in range(1, chips)]
        far = [other_core(x) for x in near]
        down_parts = expert_rows(order, near + far, gain, gate_t, up_t, down)
        core_part = other_core(down_parts[:chips])
        sums = down_parts[chips:].astype(f32) + core_part.astype(f32)
        total = sums[0]
        for by in range(1, chips):
            total = total + next_chip(sums[by].astype(bf16), by).astype(f32)
        total = total.astype(bf16)
        returned.append(total[:part])
        returned += [
            rotated(total[d * part : (d + 1) * part], "sp", -d) for d in range(1, experts)
        ]
    returned = jnp.concatenate(returned, axis=0)
    results = jnp.dot(put, returned, preferred_element_type=f32)
    merged = stream
    for k in range(top_count):
        merged = merged + route_weights[:, k : k + 1] * results[k * tokens : (k + 1) * tokens]
    return merged.astype(bf16)


def solution(mesh):
    placed = (
        P("tp", "sp"),
        P("tp", "sp"),
        P("tp", "sp"),
        P(None, "tp"),
        P("sp"),
        P("sp", None),
        P("tp", None),
        P(),
        P("sp", None),
        P("sp", None),
        P("sp", None, "tp"),
        P("sp", None, "tp"),
        P("sp", "tp", None),
    )
    return jax.shard_map(
        shards, mesh=mesh, in_specs=placed, out_specs=P("sp", "tp"), check_vma=False
    )
```

```python
import jax
import jax.numpy as jnp
from jax import lax
from jax.experimental import pallas as pl
from jax.experimental.pallas import tpu as pltpu
from jax.sharding import PartitionSpec as P

EPSILON = 1e-06


def shifted(x, axis, by):
    count = lax.axis_size(axis)
    pairs = [(i, i + by) for i in range(count) if 0 <= i + by < count]
    return lax.ppermute(x, axis, pairs)


def paired(x, axis, by):
    return lax.ppermute(x, axis, [(i, i ^ by) for i in range(lax.axis_size(axis))])


def other_core(x):
    return lax.ppermute(x, "tp", [(i, i ^ 1) for i in range(lax.axis_size("tp"))])


def next_chip(x, by):
    count = lax.axis_size("tp")
    return lax.ppermute(x, "tp", [(i, (i + 2 * by) % count) for i in range(count)])


def expert_kernel(order_ref, *refs):
    pieces = len(refs) - 10
    x_refs = refs[:pieces]
    gain_ref, gate_hbm, up_hbm, down_hbm, out_ref = refs[pieces : pieces + 5]
    gate_ref, up_ref, down_ref, first_sem, last_sem = refs[pieces + 5 :]
    tiles, size = gate_ref.shape[:2]
    width = x_refs[0].shape[1]

    first, last = [], []
    for f in range(tiles):
        for k, (hbm, ref) in enumerate(((gate_hbm, gate_ref), (up_hbm, up_ref))):
            copy = pltpu.make_async_copy(
                hbm.at[pl.ds(f * size, size)], ref.at[f], first_sem.at[2 * f + k]
            )
            copy.start()
            first.append(copy)
    for j in range(pieces):
        at = pl.multiple_of(order_ref[pieces + j] * width, width)
        copy = pltpu.make_async_copy(down_hbm.at[:, pl.ds(at, width)], down_ref.at[j], last_sem.at[j])
        copy.start()
        last.append(copy)

    total = sum(
        jnp.sum(jnp.square(x[...].astype(jnp.float32)), axis=1, keepdims=True) for x in x_refs
    )
    inv_rms = lax.rsqrt(total / (pieces * width) + EPSILON)

    def run(rows_ref, hidden_ref):
        for j, x in enumerate(x_refs):
            block = order_ref[j]
            normed = x[...].astype(jnp.float32) * inv_rms * gain_ref[block].astype(jnp.float32)
            rows_ref[block] = normed.astype(jnp.bfloat16).T
        rows = rows_ref[...].reshape(pieces * width, -1)
        for f in range(tiles):
            first[2 * f].wait()
            gate_sum = jnp.dot(gate_ref[f], rows, preferred_element_type=jnp.float32)
            first[2 * f + 1].wait()
            up_sum = jnp.dot(up_ref[f], rows, preferred_element_type=jnp.float32)
            hidden = gate_sum / (1.0 + jnp.exp(-gate_sum)) * up_sum
            hidden_ref[f] = hidden.astype(jnp.bfloat16).T
        for j in range(pieces):
            last[j].wait()
            out_ref[j] = sum(
                jnp.dot(
                    hidden_ref[f],
                    down_ref[j, f * size : (f + 1) * size, :],
                    preferred_element_type=jnp.float32,
                )
                for f in range(tiles)
            ).astype(jnp.bfloat16)

    rows_count = x_refs[0].shape[0]
    pl.run_scoped(
        run,
        pltpu.VMEM((pieces, width, rows_count), jnp.bfloat16),
        pltpu.VMEM((tiles, rows_count, size), jnp.bfloat16),
    )


def expert_rows(order, xs, gain, gate_t, up_t, down):
    pieces = len(xs)
    rows, width = xs[0].shape
    units, model_width = gate_t.shape
    tiles = next((t for t in (3, 2) if units % (16 * t) == 0), 1)
    size = units // tiles
    vmem = pl.BlockSpec(memory_space=pltpu.VMEM)
    hbm = pl.BlockSpec(memory_space=pl.ANY)
    return pl.pallas_call(
        expert_kernel,
        out_shape=jax.ShapeDtypeStruct((pieces, rows, width), jnp.bfloat16),
        in_specs=[pl.BlockSpec(memory_space=pltpu.SMEM)] + [vmem] * (pieces + 1) + [hbm] * 3,
        out_specs=vmem,
        scratch_shapes=[
            pltpu.VMEM((tiles, size, model_width), jnp.bfloat16),
            pltpu.VMEM((tiles, size, model_width), jnp.bfloat16),
            pltpu.VMEM((pieces, units, width), jnp.bfloat16),
            pltpu.SemaphoreType.DMA((2 * tiles,)),
            pltpu.SemaphoreType.DMA((pieces,)),
        ],
        cost_estimate=pl.CostEstimate(
            flops=6 * rows * units * model_width,
            bytes_accessed=6 * units * model_width,
            transcendentals=rows * units,
        ),
    )(order, *xs, gain, gate_t, up_t, down)


def shards(
    in_gate,
    out_gate,
    values,
    conv_taps,
    doc_ids,
    residual,
    out_weight,
    norm_gain,
    routes,
    route_weights,
    expert_gate,
    expert_up,
    expert_down,
):
    bf16, f32 = jnp.bfloat16, jnp.float32
    tp_count = lax.axis_size("tp")
    chips = tp_count // 2
    experts = lax.axis_size("sp")
    me = lax.axis_index("tp")
    chip, core = me // 2, me % 2
    tokens, top_count = routes.shape
    length = doc_ids.shape[0]
    model_width = residual.shape[1]
    width = model_width // tp_count

    gated_in = (in_gate.astype(f32) * values.astype(f32)).astype(bf16)
    edge = jnp.concatenate(
        [gated_in[:, -2:], jnp.broadcast_to(doc_ids[-2:].astype(bf16)[None, :], (16, 2))], axis=0
    )
    edge = shifted(edge, "sp", 1)
    channels = gated_in.shape[0]
    tail_rows, tail_docs = edge[:channels], edge[channels].astype(jnp.int32)
    extended = lax.optimization_barrier(jnp.concatenate([tail_rows, gated_in], axis=1)).astype(f32)
    docs_ext = jnp.concatenate([tail_docs, doc_ids])
    near_mask = (docs_ext[1 : length + 1] == doc_ids).astype(f32)
    far_mask = (docs_ext[0:length] == doc_ids).astype(f32)
    taps = conv_taps.astype(f32)
    convolved = (
        taps[2][:, None] * extended[:, 2:]
        + taps[1][:, None] * extended[:, 1 : length + 1] * near_mask[None, :]
        + taps[0][:, None] * extended[:, 0:length] * far_mask[None, :]
    )
    mixed_rows = (out_gate.astype(f32) * convolved).astype(bf16)
    partial = lax.dot_general(
        mixed_rows, out_weight, (((0,), (0,)), ((), ())), preferred_element_type=f32
    ).astype(bf16)

    def of_core(which):
        even = jnp.concatenate(
            [partial[:, (2 * y) * width : (2 * y + 1) * width] for y in range(chips)], axis=1
        )
        odd = jnp.concatenate(
            [partial[:, (2 * y + 1) * width : (2 * y + 2) * width] for y in range(chips)], axis=1
        )
        return jnp.where(which == 0, even, odd)

    from_core = other_core(of_core(1 - core))
    chip_sum = of_core(core).astype(f32) + from_core.astype(f32)

    def of_chip(which):
        return lax.dynamic_slice_in_dim(chip_sum, which * width, width, 1)

    projected = of_chip(chip)
    for by in range(1, chips):
        projected = projected + next_chip(of_chip((chip + by) % chips).astype(bf16), by).astype(f32)
    stream = (
        lax.dynamic_slice_in_dim(residual, me * width, width, 1).astype(f32) + projected
    )

    capacity = 3 * tokens * top_count // (2 * experts)
    chunks = [[d for d in range(experts) if (d >> 1) % 2 == c] for c in range(2)]
    chunks = [c for c in chunks if c]
    listed = [d for c in chunks for d in c]
    names = jnp.arange(experts, dtype=jnp.int32)
    hits = sum((routes[:, k : k + 1] == names[None, :]).astype(f32) for k in range(top_count))
    positions = jnp.arange(tokens, dtype=jnp.int32)
    before = (positions[None, :] < positions[:, None]).astype(bf16)
    earlier = jnp.dot(before, hits.astype(bf16), preferred_element_type=f32)
    away = routes ^ lax.axis_index("sp")
    place = (away & 1) + ((away >> 2) << 1) + ((away >> 1) & 1) * len(chunks[0])
    slots = []
    for k in range(top_count):
        rank = jnp.sum(
            jnp.where(routes[:, k : k + 1] == names[None, :], earlier, 0.0), axis=1
        ).astype(jnp.int32)
        slots.append(place[:, k] * capacity + rank)
    slot_count = experts * capacity
    places = jnp.arange(slot_count, dtype=jnp.int32)
    pick = sum((slot[None, :] == places[:, None]).astype(f32) for slot in slots).astype(bf16)
    put = jnp.concatenate(
        [(slot[:, None] == places[None, :]) for slot in slots], axis=0
    ).astype(bf16)
    pick, put = lax.optimization_barrier((pick, put))

    stream_low = stream.astype(bf16)
    steps = jnp.arange(chips, dtype=jnp.int32)
    came_from = ((chip - steps) % chips) * 2
    goes_to = ((chip + steps) % chips) * 2
    order = jnp.concatenate(
        [came_from + core, came_from + (1 - core), goes_to + (1 - core), goes_to + core]
    ).astype(jnp.int32)
    gain = norm_gain.reshape(tp_count, 1, width)
    gate_t = expert_gate[0].T
    up_t = expert_up[0].T
    down = expert_down[0]

    returned = []
    start = 0
    for chunk in chunks:
        size = len(chunk) * capacity
        picked = jnp.dot(
            pick[start : start + size], stream_low, preferred_element_type=f32
        ).astype(bf16)
        start += size

        def exchange(x):
            pieces = [x[j * capacity : (j + 1) * capacity] for j in range(len(chunk))]
            return [paired(p, "sp", d) if d else p for d, p in zip(chunk, pieces)]

        own = jnp.concatenate(exchange(picked), axis=0)
        near = [own] + [next_chip(own, by) for by in range(1, chips)]
        far = [other_core(x) for x in near]
        down_parts = expert_rows(order, near + far, gain, gate_t, up_t, down)
        core_part = other_core(down_parts[:chips])
        sums = down_parts[chips:].astype(f32) + core_part.astype(f32)
        total = sums[0]
        for by in range(1, chips):
            total = total + next_chip(sums[by].astype(bf16), by).astype(f32)
        returned += exchange(total.astype(bf16))
    returned = jnp.concatenate(returned, axis=0)
    results = jnp.dot(put, returned, preferred_element_type=f32)
    merged = stream
    for k in range(top_count):
        merged = merged + route_weights[:, k : k + 1] * results[k * tokens : (k + 1) * tokens]
    return merged.astype(bf16)


def solution(mesh):
    placed = (
        P("tp", "sp"),
        P("tp", "sp"),
        P("tp", "sp"),
        P(None, "tp"),
        P("sp"),
        P("sp", None),
        P("tp", None),
        P(),
        P("sp", None),
        P("sp", None),
        P("sp", None, "tp"),
        P("sp", None, "tp"),
        P("sp", "tp", None),
    )
    return jax.shard_map(
        shards, mesh=mesh, in_specs=placed, out_specs=P("sp", "tp"), check_vma=False
    )
```
